256 devices in a mesh: grp: 2 (over y), ep: 64 (over z, x), tp: 2 (over core).
Axes of the slice: x: 4, y: 2, z: 16, core: 2. Of those that a mesh axis runs over, the one named last changes fastest.
The devices are a block of a 4x16x16 slice.
Arguments:
- tokens: bfloat16 [32768, 2048], P(('grp', 'ep'), 'tp'), parts along dimension 0, may hold values from -6 to 6
- norm_gain: bfloat16 [2048], P('tp'), may hold values from 0.099609375 to 1.8984375
- w_gate: bfloat16 [64, 2048, 1024], P('ep', None, 'tp'), may hold values from -0.125 to 0.125
- w_up: bfloat16 [64, 2048, 1024], P('ep', None, 'tp'), may hold values from -0.125 to 0.125
- w_down: bfloat16 [64, 1024, 2048], P('ep', 'tp'), may hold values from -0.1875 to 0.1875
- expert_ids: int32 [32768, 2], P(('grp', 'ep')), parts along dimension 0, may hold values from 0 to 63, as said below
- combine: float32 [32768, 2], P(('grp', 'ep')), parts along dimension 0, may hold values from 0.1 to 1
- final_gain: bfloat16 [2048], P('tp'), may hold values from 0.099609375 to 1.8984375
Outputs:
- result: bfloat16 [32768, 2048], P(('grp', 'ep'), 'tp'), parts along dimension 0
The draws below stay inside these ranges and needn't reach their ends.
There are 2 independent parts, one for each index of `grp`. The reference program is written for one: setup_inputs(seed, part) draws one part's arguments, and reference() takes and returns one part's arrays. A program takes and returns all parts, laid end to end along the dimension named above; an argument that names none is the same for every part. Nothing has to cross between parts.
Inputs may be any that keep to these rules, and one draw needn't show every extreme that they name: `expert_ids`: the experts form 4 groups of consecutive ids of equal size; the 2 experts of a row are different and lie in one group. Among the rows of one index of ep no expert is named more than 20 times, and in each such block some expert is named exactly 20 times.
All inputs are finite; a program needn't handle non-finite values.
Results may differ from the reference program's by a relative error of at most 0.0077.
Values may be sent and summed in bfloat16 or wider, within the bound.
No kernel may reach another device: no remote copies, remote signals or barrier semaphores. Data moves between devices by JAX's collectives and lax.ppermute only.
A program may use at most 64 MiB of HBM per device.

```python
import math
import jax
import jax.numpy as jnp
from jax import lax

D = 2048
FF = 1024
GROUPS = 4
TOP = 2
TOK_DEV = 256
EXPERTS = 64
CAP = 20
TOKENS = 16384
N_EP = 64
N_TP = 2


def draw_expert_ids(key, part):
    per_group = EXPERTS // GROUPS
    base = TOK_DEV // 8

    def one_block(block_key):
        key_busy, key_order, key_shift = jax.random.split(block_key, 3)
        busy = jax.random.randint(key_busy, (), 0, GROUPS)
        labels = jnp.arange(GROUPS, dtype=jnp.int32)
        counts = jnp.where(labels == busy, 5 * base, base).astype(jnp.int32)
        starts = jnp.cumsum(counts) - counts
        order = jax.random.permutation(key_order, TOK_DEV)
        ranks = jnp.arange(TOK_DEV, dtype=jnp.int32)
        group = jnp.sum((ranks[:, None] >= (starts + counts)[None, :]).astype(jnp.int32), axis=1)
        inner = ranks - starts[group]
        shifts = jax.random.randint(key_shift, (GROUPS,), 0, per_group)[group]
        first = (inner + shifts) % per_group
        second = (first + 1 + inner // per_group % max(per_group - 1, 1)) % per_group
        paired = jnp.stack([group * per_group + first, group * per_group + second], axis=1).astype(jnp.int32)
        return jnp.zeros((TOK_DEV, 2), jnp.int32).at[order].set(paired)
    blocks = jax.vmap(one_block)(jax.random.split(jax.random.fold_in(key, 11), TOKENS // TOK_DEV))
    return blocks.reshape(TOKENS, 2)


def block_scale(key, dims, cuts, low, high):
    loudness, own = 1.0, jax.random.fold_in(key, 6)
    for dim, blocks in cuts:
        steps = jnp.exp(jax.random.uniform(jax.random.fold_in(own, dim), (blocks,), jnp.float32, low / len(cuts), high / len(cuts)))
        loudness = loudness * jnp.repeat(steps, dims[dim] // blocks).reshape([-1 if axis == dim else 1 for axis in range(len(dims))])
    return loudness


def scatter_about(rng, dims, deviation, reach, cuts=(), held_as=jnp.bfloat16):
    array = deviation * jax.random.normal(rng, dims, jnp.float32)
    if cuts:
        array = array * block_scale(rng, dims, cuts, -0.22, 0.18)
    return jnp.clip(array, -reach, reach).astype(held_as)


def setup_inputs(seed: int = 0, part: int = 0) -> dict:
    key_of = jax.random.split(jax.random.key(seed), 9)
    own_keys = jax.random.split(jax.random.fold_in(key_of[8], part), 9)
    tokens = scatter_about(own_keys[0], (TOKENS, D), 1.0, 6.0, ((0, 64), (1, 2)))
    norm_gain = jnp.clip(1.0 + 0.18 * jax.random.normal(key_of[1], (D,), jnp.float32), 0.099609375, 1.8984375).astype(jnp.bfloat16)
    w_gate = scatter_about(key_of[2], (EXPERTS, D, FF), D ** -0.5, 0.125, ((0, 64), (2, 2)))
    w_up = scatter_about(key_of[3], (EXPERTS, D, FF), D ** -0.5, 0.125, ((0, 64), (2, 2)))
    w_down = scatter_about(key_of[4], (EXPERTS, FF, D), FF ** -0.5, 0.1875, ((0, 64), (1, 2)))
    expert_ids = draw_expert_ids(jax.random.fold_in(jax.random.fold_in(key_of[8], part), 71), part)
    combine = jnp.clip(jnp.exp(math.log(1.0) - 2.3025851 * jax.random.uniform(own_keys[6], (TOKENS, TOP), jnp.float32) ** block_scale(own_keys[6], (TOKENS, TOP), ((0, 64),), -0.2, 0.2)), 0.1, 1.0)
    final_gain = jnp.clip(1.0 + 0.18 * jax.random.normal(key_of[7], (D,), jnp.float32), 0.099609375, 1.8984375).astype(jnp.bfloat16)
    return dict(tokens=tokens, norm_gain=norm_gain, w_gate=w_gate, w_up=w_up, w_down=w_down, expert_ids=expert_ids, combine=combine, final_gain=final_gain)


def reference(tokens, norm_gain, w_gate, w_up, w_down, expert_ids, combine, final_gain):
    eps = 1e-06
    xf = tokens.astype(jnp.float32)
    normed = (xf * lax.rsqrt(lax.optimization_barrier(jnp.mean(xf * xf, axis=-1, keepdims=True)) + eps) * norm_gain.astype(jnp.float32)).astype(jnp.bfloat16)
    flat = expert_ids.reshape(-1)
    weights = combine.reshape(-1)
    limit = N_EP * CAP
    half_ff = FF // N_TP

    def step(acc, expert):
        hits = flat == expert
        pos = jnp.nonzero(hits, size=limit, fill_value=0)[0].astype(jnp.int32)
        live = jnp.arange(limit, dtype=jnp.int32) < jnp.sum(hits.astype(jnp.int32))
        owner = pos // TOP
        rows = normed[owner].astype(jnp.float32)
        gate_w = lax.dynamic_index_in_dim(w_gate, expert, 0, keepdims=False).astype(jnp.float32)
        up_w = lax.dynamic_index_in_dim(w_up, expert, 0, keepdims=False).astype(jnp.float32)
        down_w = lax.dynamic_index_in_dim(w_down, expert, 0, keepdims=False).astype(jnp.float32)
        gate = jnp.dot(rows, gate_w, preferred_element_type=jnp.float32)
        upper = jnp.dot(rows, up_w, preferred_element_type=jnp.float32)
        hidden = (jax.nn.silu(gate) * upper).astype(jnp.bfloat16)
        parts = jnp.einsum('rjf,jfd->jrd', hidden.astype(jnp.float32).reshape(limit, N_TP, half_ff), down_w.reshape(N_TP, half_ff, D)).astype(jnp.bfloat16)
        parts = lax.optimization_barrier(parts)
        summed = lax.optimization_barrier(jnp.sum(parts.astype(jnp.float32), axis=0)).astype(jnp.bfloat16)
        summed = lax.optimization_barrier(summed)
        scale = jnp.where(live, weights[pos], jnp.float32(0.0))
        acc = acc.at[owner].add(scale[:, None] * summed.astype(jnp.float32))
        return (acc, None)
    mixed, _ = lax.scan(step, jnp.zeros((TOKENS, D), jnp.float32), jnp.arange(EXPERTS, dtype=jnp.int32))
    norm = lax.rsqrt(lax.optimization_barrier(jnp.mean(mixed * mixed, axis=-1, keepdims=True)) + eps)
    return (mixed * norm * final_gain.astype(jnp.float32)).astype(jnp.bfloat16)
```

```python
import functools

import jax
import jax.numpy as jnp
from jax import lax
from jax.experimental import pallas as pl
from jax.experimental.pallas import tpu as pltpu
from jax.sharding import PartitionSpec as P

GROUPS = 4
EPS = 1e-06
LANES = 128
VMEM_LIMIT = 60 * 1024 * 1024


def dispatch_kernel(ids_ref, tok_ref, out_ref, pos_ref, tiles_ref, count_ref, *, capacity):
    tok_dev, half = tok_ref.shape
    sub = half // LANES
    top = ids_ref.shape[0]
    for j in range(sub):
        block = tok_ref[:, j * LANES : (j + 1) * LANES].astype(jnp.float32)
        tiles_ref[pl.ds(j, tok_dev, stride=sub), :] = block

    def clear(e, carry):
        count_ref[e] = 0
        return carry

    lax.fori_loop(0, count_ref.shape[0], clear, 0)

    def place(t, carry):
        row = tiles_ref[pl.ds(pl.multiple_of(t * sub, sub), sub), :].astype(jnp.bfloat16)
        for k in range(top):
            e = ids_ref[k, t]
            rank = count_ref[e]
            count_ref[e] = rank + 1
            slot = e * capacity + rank
            pos_ref[k, t] = slot
            out_ref[slot] = row
        return carry

    lax.fori_loop(0, tok_dev, place, 0, unroll=8)


def dispatch(ids, tokens, experts, capacity):
    tok_dev, half = tokens.shape
    sub = half // LANES
    return pl.pallas_call(
        functools.partial(dispatch_kernel, capacity=capacity),
        out_shape=(
            jax.ShapeDtypeStruct((experts * capacity, sub, LANES), jnp.bfloat16),
            jax.ShapeDtypeStruct(ids.shape, jnp.int32),
        ),
        in_specs=[
            pl.BlockSpec(memory_space=pltpu.SMEM),
            pl.BlockSpec(memory_space=pltpu.VMEM),
        ],
        out_specs=(
            pl.BlockSpec(memory_space=pltpu.VMEM),
            pl.BlockSpec(memory_space=pltpu.SMEM),
        ),
        scratch_shapes=[
            pltpu.VMEM((tok_dev * sub, LANES), jnp.float32),
            pltpu.SMEM((experts,), jnp.int32),
        ],
        compiler_params=pltpu.CompilerParams(vmem_limit_bytes=VMEM_LIMIT),
        name="dispatch",
    )(ids, tokens)


def expert_kernel(
    arr_ref, gain_ref, wg0, wg1, wu0, wu1, wd0, wd1, out_ref,
    tiles_ref, x_ref, hid_ref, wg_ref, wu_ref, wd_ref, sems, *, n_tp, per_part, width,
):
    rows = x_ref.shape[0]
    sub = arr_ref.shape[1]
    half = sub * LANES
    sources = rows // per_part
    copies = []
    for i, (src, dst) in enumerate(
        ((wg0, wg_ref.at[0]), (wg1, wg_ref.at[1]), (wu0, wu_ref.at[0]), (wu1, wu_ref.at[1]),
         (wd0, wd_ref.at[0]), (wd1, wd_ref.at[1]))
    ):
        copy = pltpu.make_async_copy(src.at[0], dst, sems.at[i])
        copy.start()
        copies.append(copy)

    def spread(s, carry):
        for c in range(n_tp):
            part = arr_ref[pl.ds((s * n_tp + c) * per_part, per_part)].astype(jnp.float32)
            at = pl.multiple_of(s * (per_part * sub), per_part * sub)
            tiles_ref[c, pl.ds(at, per_part * sub), :] = part.reshape(per_part * sub, LANES)
        return carry

    lax.fori_loop(0, sources, spread, 0, unroll=4)

    block = 80

    def normalize(b, carry):
        def piece(c, j):
            return tiles_ref[c, pl.ds(b * (block * sub) + j, block, stride=sub), :]

        squares = jnp.zeros((block, LANES), jnp.float32)
        for c in range(n_tp):
            for j in range(sub):
                v = piece(c, j)
                squares += v * v
        scale = lax.rsqrt(jnp.sum(squares, axis=1, keepdims=True) / width + EPS)
        at = pl.ds(pl.multiple_of(b * block, block), block)
        for c in range(n_tp):
            for j in range(sub):
                lo = c * half + j * LANES
                v = piece(c, j) * scale * gain_ref[:, lo : lo + LANES]
                x_ref[at, lo : lo + LANES] = v.astype(jnp.bfloat16)
        return carry

    lax.fori_loop(0, rows // block, normalize, 0)

    ff = wg_ref.shape[2]
    step = 256
    for h in range(n_tp):
        copies[h].wait()
        copies[n_tp + h].wait()
        for n in range(ff // step):
            cols = slice(n * step, (n + 1) * step)
            gate = jnp.dot(x_ref[...], wg_ref[h, :, cols], preferred_element_type=jnp.float32)
            upper = jnp.dot(x_ref[...], wu_ref[h, :, cols], preferred_element_type=jnp.float32)
            hidden = (gate / (1.0 + jnp.exp(-gate))) * upper
            hid_ref[:, h * ff + n * step : h * ff + (n + 1) * step] = hidden.astype(jnp.bfloat16)
    for h in range(n_tp):
        copies[2 * n_tp + h].wait()
    for c in range(n_tp):
        for n in range(half // step):
            lo = c * half + n * step
            total = jnp.dot(
                hid_ref[...],
                jnp.concatenate([wd_ref[h, :, lo : lo + step] for h in range(n_tp)], axis=0),
                preferred_element_type=jnp.float32,
            )
            for i in range(step // LANES):
                j = n * (step // LANES) + i
                tiles_ref[c, pl.ds(j, rows, stride=sub), :] = total[:, i * LANES : (i + 1) * LANES]

    def gather(s, carry):
        for c in range(n_tp):
            at = pl.multiple_of(s * (per_part * sub), per_part * sub)
            part = tiles_ref[c, pl.ds(at, per_part * sub), :].reshape(per_part, sub, LANES)
            out_ref[pl.ds((s * n_tp + c) * per_part, per_part)] = part.astype(jnp.bfloat16)
        return carry

    lax.fori_loop(0, sources, gather, 0, unroll=4)


def expert(arrived, gain, gates, uppers, downs, per_part, n_tp):
    total, sub, lanes = arrived.shape
    rows = total // n_tp
    _, width, ff = gates[0].shape
    anywhere = pl.BlockSpec(memory_space=pl.ANY)
    return pl.pallas_call(
        functools.partial(expert_kernel, n_tp=n_tp, per_part=per_part, width=width),
        out_shape=jax.ShapeDtypeStruct(arrived.shape, jnp.bfloat16),
        in_specs=[pl.BlockSpec(memory_space=pltpu.VMEM), pl.BlockSpec(memory_space=pltpu.VMEM)]
        + [anywhere] * (3 * n_tp),
        out_specs=pl.BlockSpec(memory_space=pltpu.VMEM),
        scratch_shapes=[
            pltpu.VMEM((n_tp, rows * sub, lanes), jnp.float32),
            pltpu.VMEM((rows, width), jnp.bfloat16),
            pltpu.VMEM((rows, ff * n_tp), jnp.bfloat16),
            pltpu.VMEM((n_tp, width, ff), jnp.bfloat16),
            pltpu.VMEM((n_tp, width, ff), jnp.bfloat16),
            pltpu.VMEM((n_tp, ff, width), jnp.bfloat16),
            pltpu.SemaphoreType.DMA((3 * n_tp,)),
        ],
        compiler_params=pltpu.CompilerParams(vmem_limit_bytes=VMEM_LIMIT),
        cost_estimate=pl.CostEstimate(
            flops=6 * rows * width * ff * n_tp, transcendentals=rows * ff * n_tp,
            bytes_accessed=12 * width * ff + 4 * total * sub * lanes,
        ),
        name="expert",
    )(arrived, gain, *gates, *uppers, *downs)


def combine_kernel(pos_ref, mix_ref, ret_ref, out_ref, sq_ref, tiles_ref):
    top, tok_dev = pos_ref.shape
    sub = ret_ref.shape[1]

    def pick(t, carry):
        total = mix_ref[0, t] * ret_ref[pos_ref[0, t]].astype(jnp.float32)
        for k in range(1, top):
            total += mix_ref[k, t] * ret_ref[pos_ref[k, t]].astype(jnp.float32)
        tiles_ref[pl.ds(pl.multiple_of(t * sub, sub), sub), :] = total
        return carry

    lax.fori_loop(0, tok_dev, pick, 0, unroll=8)
    squares = jnp.zeros((tok_dev, LANES), jnp.float32)
    for j in range(sub):
        v = tiles_ref[pl.ds(j, tok_dev, stride=sub), :]
        out_ref[:, j * LANES : (j + 1) * LANES] = v
        squares += v * v
    sq_ref[...] = jnp.sum(squares, axis=1, keepdims=True)


def combined(pos, mix, returned):
    _, tok_dev = pos.shape
    _, sub, lanes = returned.shape
    return pl.pallas_call(
        combine_kernel,
        out_shape=(
            jax.ShapeDtypeStruct((tok_dev, sub * lanes), jnp.float32),
            jax.ShapeDtypeStruct((tok_dev, 1), jnp.float32),
        ),
        in_specs=[
            pl.BlockSpec(memory_space=pltpu.SMEM),
            pl.BlockSpec(memory_space=pltpu.SMEM),
            pl.BlockSpec(memory_space=pltpu.VMEM),
        ],
        out_specs=(
            pl.BlockSpec(memory_space=pltpu.VMEM),
            pl.BlockSpec(memory_space=pltpu.VMEM),
        ),
        scratch_shapes=[pltpu.VMEM((tok_dev * sub, lanes), jnp.float32)],
        compiler_params=pltpu.CompilerParams(vmem_limit_bytes=VMEM_LIMIT),
        name="combine",
    )(pos, mix, returned)


def body(tokens, norm_gain, w_gate, w_up, w_down, expert_ids, combine, final_gain):
    tok_dev, half = tokens.shape
    n_ep = lax.axis_size("ep")
    n_tp = lax.axis_size("tp")
    width = half * n_tp
    experts = w_gate.shape[0] * n_ep
    capacity = tok_dev // 8 * 5 * 2 // (experts // GROUPS)
    per_part = capacity // n_tp
    sub = half // LANES

    swap = [(i, (i + 1) % n_tp) for i in range(n_tp)]
    others = [lax.ppermute(w, "tp", swap) for w in (w_gate, w_up, w_down)]
    gain = lax.all_gather(norm_gain.astype(jnp.float32), "tp", tiled=True)[None, :]

    outgoing, pos = dispatch(expert_ids.T, tokens, experts, capacity)
    shape = (n_ep * n_tp, per_part, sub, LANES)
    arrived = lax.all_to_all(
        outgoing.reshape(shape), ("ep", "tp"), split_axis=0, concat_axis=0, tiled=True
    )
    results = expert(
        arrived.reshape(-1, sub, LANES), gain, (w_gate, others[0]), (w_up, others[1]),
        (w_down, others[2]), per_part, n_tp,
    )
    returned = lax.all_to_all(
        results.reshape(shape), ("ep", "tp"), split_axis=0, concat_axis=0, tiled=True
    )
    mixed, squares = combined(pos, combine.T, returned.reshape(-1, sub, LANES))
    totals = lax.all_gather(squares[:, 0], "tp").sum(axis=0)
    norm = lax.rsqrt(totals[:, None] / width + EPS)
    return (mixed * norm * final_gain.astype(jnp.float32)).astype(jnp.bfloat16)


def solution(mesh):
    placed = (
        P(("grp", "ep"), "tp"),
        P("tp"),
        P("ep", None, "tp"),
        P("ep", None, "tp"),
        P("ep", "tp", None),
        P(("grp", "ep"), None),
        P(("grp", "ep"), None),
        P("tp"),
    )
    return jax.shard_map(
        body, mesh=mesh, in_specs=placed, out_specs=P(("grp", "ep"), "tp"), check_vma=False
    )
```

```python
import functools

import jax
import jax.numpy as jnp
from jax import lax
from jax.experimental import pallas as pl
from jax.experimental.pallas import tpu as pltpu
from jax.sharding import PartitionSpec as P

GROUPS = 4
EPS = 1e-06
LANES = 128
DISPATCH_VMEM = 60 * 1024 * 1024
EXPERT_VMEM = 40 * 1024 * 1024
COMBINE_VMEM = 8 * 1024 * 1024


def dispatch_kernel(ids_ref, tok_ref, out_ref, pos_ref, tiles_ref, next_ref, *, capacity):
    tok_dev, half = tok_ref.shape
    sub = half // LANES
    top = ids_ref.shape[0]
    for j in range(sub):
        block = tok_ref[:, j * LANES : (j + 1) * LANES].astype(jnp.float32)
        tiles_ref[pl.ds(j, tok_dev, stride=sub), :] = block

    for e in range(next_ref.shape[0]):
        next_ref[e] = e * capacity

    def place(t, carry):
        row = tiles_ref[pl.ds(pl.multiple_of(t * sub, sub), sub), :].astype(jnp.bfloat16)
        for k in range(top):
            e = ids_ref[k, t]
            slot = next_ref[e]
            next_ref[e] = slot + 1
            pos_ref[k, t] = slot
            out_ref[slot] = row
        return carry

    lax.fori_loop(0, tok_dev, place, 0, unroll=8)


def dispatch(ids, tokens, experts, capacity):
    tok_dev, half = tokens.shape
    sub = half // LANES
    return pl.pallas_call(
        functools.partial(dispatch_kernel, capacity=capacity),
        out_shape=(
            jax.ShapeDtypeStruct((experts * capacity, sub, LANES), jnp.bfloat16),
            jax.ShapeDtypeStruct(ids.shape, jnp.int32),
        ),
        in_specs=[
            pl.BlockSpec(memory_space=pltpu.SMEM),
            pl.BlockSpec(memory_space=pltpu.VMEM),
        ],
        out_specs=(
            pl.BlockSpec(memory_space=pltpu.VMEM),
            pl.BlockSpec(memory_space=pltpu.SMEM),
        ),
        scratch_shapes=[
            pltpu.VMEM((tok_dev * sub, LANES), jnp.float32),
            pltpu.SMEM((experts,), jnp.int32),
        ],
        compiler_params=pltpu.CompilerParams(vmem_limit_bytes=DISPATCH_VMEM),
        name="dispatch",
    )(ids, tokens)


def expert_kernel(
    arr_ref, gain_ref, wg0, wg1, wu0, wu1, wd0, wd1, out_ref,
    tiles_ref, x_ref, hid_ref, wg_ref, wu_ref, wd_ref, rows_ref, sems, out_sems,
    *, n_tp, per_part, width,
):
    rows = x_ref.shape[0]
    sub = arr_ref.shape[1]
    half = sub * LANES
    sources = rows // per_part
    copies = []
    for i, (src, dst) in enumerate(
        ((wg0, wg_ref.at[0]), (wu0, wu_ref.at[0]), (wg1, wg_ref.at[1]), (wu1, wu_ref.at[1]),
         (wd0, wd_ref.at[0]), (wd1, wd_ref.at[1]))
    ):
        copy = pltpu.make_async_copy(src.at[0], dst, sems.at[i])
        copy.start()
        copies.append(copy)

    def spread(s, carry):
        for c in range(n_tp):
            part = arr_ref[pl.ds((s * n_tp + c) * per_part, per_part)].astype(jnp.float32)
            at = pl.multiple_of(s * (per_part * sub), per_part * sub)
            tiles_ref[c, pl.ds(at, per_part * sub), :] = part.reshape(per_part * sub, LANES)
        return carry

    lax.fori_loop(0, sources, spread, 0, unroll=8)

    block = 80

    def normalize(b, carry):
        def piece(c, j):
            return tiles_ref[c, pl.ds(b * (block * sub) + j, block, stride=sub), :]

        squares = jnp.zeros((block, LANES), jnp.float32)
        for c in range(n_tp):
            for j in range(sub):
                v = piece(c, j)
                squares += v * v
        scale = lax.rsqrt(jnp.sum(squares, axis=1, keepdims=True) / width + EPS)
        at = pl.ds(pl.multiple_of(b * block, block), block)
        for c in range(n_tp):
            for j in range(sub):
                lo = c * half + j * LANES
                v = piece(c, j) * scale * gain_ref[:, lo : lo + LANES]
                x_ref[at, lo : lo + LANES] = v.astype(jnp.bfloat16)
        return carry

    lax.fori_loop(0, rows // block, normalize, 0)

    ff = wg_ref.shape[2]
    step = 256
    for h in range(n_tp):
        copies[2 * h].wait()
        copies[2 * h + 1].wait()
        for n in range(ff // step):
            cols = slice(n * step, (n + 1) * step)
            gate = jnp.dot(x_ref[...], wg_ref[h, :, cols], preferred_element_type=jnp.float32)
            upper = jnp.dot(x_ref[...], wu_ref[h, :, cols], preferred_element_type=jnp.float32)
            hidden = (gate / (1.0 + jnp.exp(-gate))) * upper
            hid_ref[:, h * ff + n * step : h * ff + (n + 1) * step] = hidden.astype(jnp.bfloat16)
    for h in range(n_tp):
        copies[2 * n_tp + h].wait()
    sends = []
    for c in range(n_tp):
        for n in range(half // step):
            lo = c * half + n * step
            total = jnp.dot(
                hid_ref[...],
                jnp.concatenate([wd_ref[h, :, lo : lo + step] for h in range(n_tp)], axis=0),
                preferred_element_type=jnp.float32,
            )
            for i in range(step // LANES):
                j = n * (step // LANES) + i
                tiles_ref[c, pl.ds(j, rows, stride=sub), :] = total[:, i * LANES : (i + 1) * LANES]

        def gather(s, carry):
            at = pl.multiple_of(s * (per_part * sub), per_part * sub)
            part = tiles_ref[c, pl.ds(at, per_part * sub), :].reshape(per_part, sub, LANES)
            rows_ref[c, s] = part.astype(jnp.bfloat16)
            return carry

        lax.fori_loop(0, sources, gather, 0, unroll=8)
        sends.append(pltpu.make_async_copy(rows_ref.at[c], out_ref.at[:, c], out_sems.at[c]))
        sends[c].start()
    for send in sends:
        send.wait()


def in_vmem(x):
    return pltpu.with_memory_space_constraint(x, pltpu.VMEM)


def in_hbm(x):
    return pltpu.with_memory_space_constraint(x, pltpu.HBM)


def expert(arrived, gain, gates, uppers, downs, per_part, n_tp):
    total, sub, lanes = arrived.shape
    rows = total // n_tp
    _, width, ff = gates[0].shape
    anywhere = pl.BlockSpec(memory_space=pltpu.HBM)
    return pl.pallas_call(
        functools.partial(expert_kernel, n_tp=n_tp, per_part=per_part, width=width),
        out_shape=pltpu.HBM((rows // per_part, n_tp, per_part, sub, lanes), jnp.bfloat16),
        in_specs=[pl.BlockSpec(memory_space=pltpu.VMEM), pl.BlockSpec(memory_space=pltpu.VMEM)]
        + [anywhere] * (3 * n_tp),
        out_specs=pl.BlockSpec(memory_space=pltpu.HBM),
        scratch_shapes=[
            pltpu.VMEM((n_tp, rows * sub, lanes), jnp.float32),
            pltpu.VMEM((rows, width), jnp.bfloat16),
            pltpu.VMEM((rows, ff * n_tp), jnp.bfloat16),
            pltpu.VMEM((n_tp, width, ff), jnp.bfloat16),
            pltpu.VMEM((n_tp, width, ff), jnp.bfloat16),
            pltpu.VMEM((n_tp, ff, width), jnp.bfloat16),
            pltpu.VMEM((n_tp, rows // per_part, per_part, sub, lanes), jnp.bfloat16),
            pltpu.SemaphoreType.DMA((3 * n_tp,)),
            pltpu.SemaphoreType.DMA((n_tp,)),
        ],
        compiler_params=pltpu.CompilerParams(vmem_limit_bytes=EXPERT_VMEM),
        cost_estimate=pl.CostEstimate(
            flops=6 * rows * width * ff * n_tp, transcendentals=rows * ff * n_tp,
            bytes_accessed=12 * width * ff + 4 * total * sub * lanes,
        ),
        name="expert",
    )(in_vmem(arrived), gain, *[in_hbm(w) for w in (*gates, *uppers, *downs)])


def combine_kernel(pos_ref, mix_ref, ret_ref, out_ref, sq_ref, tiles_ref):
    top, tok_dev = pos_ref.shape
    sub = ret_ref.shape[1]

    def pick(t, carry):
        total = mix_ref[0, t] * ret_ref[pos_ref[0, t]].astype(jnp.float32)
        for k in range(1, top):
            total += mix_ref[k, t] * ret_ref[pos_ref[k, t]].astype(jnp.float32)
        tiles_ref[pl.ds(pl.multiple_of(t * sub, sub), sub), :] = total
        return carry

    lax.fori_loop(0, tok_dev, pick, 0, unroll=8)
    squares = jnp.zeros((tok_dev, LANES), jnp.float32)
    for j in range(sub):
        v = tiles_ref[pl.ds(j, tok_dev, stride=sub), :]
        out_ref[:, j * LANES : (j + 1) * LANES] = v
        squares += v * v
    sq_ref[...] = jnp.sum(squares, axis=1, keepdims=True)


def combined(pos, mix, returned):
    _, tok_dev = pos.shape
    _, sub, lanes = returned.shape
    return pl.pallas_call(
        combine_kernel,
        out_shape=(
            pltpu.VMEM((tok_dev, sub * lanes), jnp.float32),
            jax.ShapeDtypeStruct((tok_dev, 1), jnp.float32),
        ),
        in_specs=[
            pl.BlockSpec(memory_space=pltpu.SMEM),
            pl.BlockSpec(memory_space=pltpu.SMEM),
            pl.BlockSpec(memory_space=pltpu.VMEM),
        ],
        out_specs=(
            pl.BlockSpec(memory_space=pltpu.VMEM),
            pl.BlockSpec(memory_space=pltpu.VMEM),
        ),
        scratch_shapes=[pltpu.VMEM((tok_dev * sub, lanes), jnp.float32)],
        compiler_params=pltpu.CompilerParams(vmem_limit_bytes=COMBINE_VMEM),
        name="combine",
    )(pos, mix, in_vmem(returned))


def finish_kernel(mix_ref, tot_ref, gain_ref, out_ref, *, width):
    totals = jnp.sum(tot_ref[...], axis=0)
    norm = lax.rsqrt(totals / width + EPS)
    out_ref[...] = (mix_ref[...] * norm * gain_ref[...].astype(jnp.float32)).astype(jnp.bfloat16)


def finished(mixed, totals, gain, width):
    return pl.pallas_call(
        functools.partial(finish_kernel, width=width),
        out_shape=jax.ShapeDtypeStruct(mixed.shape, jnp.bfloat16),
        in_specs=[pl.BlockSpec(memory_space=pltpu.VMEM)] * 3,
        out_specs=pl.BlockSpec(memory_space=pltpu.VMEM),
        compiler_params=pltpu.CompilerParams(vmem_limit_bytes=COMBINE_VMEM),
        name="finish",
    )(in_vmem(mixed), totals, gain[None, :])


def body(tokens, norm_gain, w_gate, w_up, w_down, expert_ids, combine, final_gain):
    tok_dev, half = tokens.shape
    n_ep = lax.axis_size("ep")
    n_tp = lax.axis_size("tp")
    width = half * n_tp
    experts = w_gate.shape[0] * n_ep
    capacity = tok_dev // 8 * 5 * 2 // (experts // GROUPS)
    per_part = capacity // n_tp
    sub = half // LANES

    swap = [(i, (i + 1) % n_tp) for i in range(n_tp)]
    others = [lax.ppermute(w, "tp", swap) for w in (w_gate, w_up, w_down)]
    gain = lax.all_gather(norm_gain.astype(jnp.float32), "tp", tiled=True)[None, :]

    outgoing, pos = dispatch(expert_ids.T, tokens, experts, capacity)
    shape = (n_ep * n_tp, per_part, sub, LANES)
    arrived = lax.all_to_all(
        outgoing.reshape(shape), ("ep", "tp"), split_axis=0, concat_axis=0, tiled=True
    )
    results = expert(
        arrived.reshape(-1, sub, LANES), gain, (w_gate, others[0]), (w_up, others[1]),
        (w_down, others[2]), per_part, n_tp,
    )
    returned = lax.all_to_all(
        results.reshape(shape), ("ep", "tp"), split_axis=0, concat_axis=0, tiled=True
    )
    mixed, squares = combined(pos, combine.T, returned.reshape(-1, sub, LANES))
    totals = lax.all_gather(squares, "tp")
    return finished(mixed, totals, final_gain, width)


def solution(mesh):
    placed = (
        P(("grp", "ep"), "tp"),
        P("tp"),
        P("ep", None, "tp"),
        P("ep", None, "tp"),
        P("ep", "tp", None),
        P(("grp", "ep"), None),
        P(("grp", "ep"), None),
        P("tp"),
    )
    return jax.shard_map(
        body, mesh=mesh, in_specs=placed, out_specs=P(("grp", "ep"), "tp"), check_vma=False
    )
```

```python
import functools

import jax
import jax.numpy as jnp
from jax import lax
from jax.experimental import pallas as pl
from jax.experimental.pallas import tpu as pltpu
from jax.sharding import Mesh
from jax.sharding import PartitionSpec as P


GROUPS = 4
ROW = 4
NEAR = 10
EPS = 1e-06
LANES = 128
DISPATCH_VMEM = 60 * 1024 * 1024
EXPERT_VMEM = 40 * 1024 * 1024
COMBINE_VMEM = 8 * 1024 * 1024


def offsets(n_z):
    return [(i + 1) // 2 if i % 2 else -(i // 2) for i in range(n_z)]


def dispatch_kernel(z_ref, ids_ref, tok_ref, *refs, capacity):
    *out_refs, pos_ref, tiles_ref, rows_ref, next_ref, sems = refs
    tok_dev, half = tok_ref.shape
    sub = half // LANES
    top = ids_ref.shape[0]
    n_z = len(out_refs)
    block = ROW * capacity
    for j in range(sub):
        part = tok_ref[:, j * LANES : (j + 1) * LANES].astype(jnp.float32)
        tiles_ref[pl.ds(j, tok_dev, stride=sub), :] = part
    z = z_ref[0]
    for row in range(n_z):
        away = row - z
        away = jnp.where(away < 0, away + n_z, away)
        place_in = jnp.where(away * 2 > n_z, 2 * (n_z - away), jnp.maximum(2 * away - 1, 0))
        for x in range(ROW):
            next_ref[row * ROW + x] = place_in * block + x * capacity

    def place(t, carry):
        row = tiles_ref[pl.ds(pl.multiple_of(t * sub, sub), sub), :].astype(jnp.bfloat16)
        for k in range(top):
            e = ids_ref[k, t]
            slot = next_ref[e]
            next_ref[e] = slot + 1
            pos_ref[k, t] = slot
            rows_ref[slot] = row
        return carry

    lax.fori_loop(0, tok_dev, place, 0, unroll=8)
    copies = []
    for i, out_ref in enumerate(out_refs):
        part = rows_ref.at[pl.ds(i * block, block)]
        copies.append(pltpu.make_async_copy(part, out_ref, sems.at[i]))
    for copy in copies:
        copy.start()
    for copy in copies:
        copy.wait()


def dispatch(z, ids, tokens, experts, capacity):
    tok_dev, half = tokens.shape
    sub = half // LANES
    n_z = experts // ROW
    return pl.pallas_call(
        functools.partial(dispatch_kernel, capacity=capacity),
        out_shape=tuple(
            pltpu.HBM((ROW * capacity, sub, LANES), jnp.bfloat16) for _ in range(n_z)
        )
        + (jax.ShapeDtypeStruct(ids.shape, jnp.int32),),
        in_specs=[
            pl.BlockSpec(memory_space=pltpu.SMEM),
            pl.BlockSpec(memory_space=pltpu.SMEM),
            pl.BlockSpec(memory_space=pltpu.VMEM),
        ],
        out_specs=tuple(pl.BlockSpec(memory_space=pltpu.HBM) for _ in range(n_z))
        + (pl.BlockSpec(memory_space=pltpu.SMEM),),
        scratch_shapes=[
            pltpu.VMEM((tok_dev * sub, LANES), jnp.float32),
            pltpu.VMEM((experts * capacity, sub, LANES), jnp.bfloat16),
            pltpu.SMEM((experts,), jnp.int32),
            pltpu.SemaphoreType.DMA((n_z,)),
        ],
        compiler_params=pltpu.CompilerParams(vmem_limit_bytes=DISPATCH_VMEM),
        name="dispatch",
    )(z, ids, tokens)


def expert_kernel(
    arr_ref, gain_ref, wg0, wg1, wu0, wu1, wd0, wd1, out_ref,
    tiles_ref, x_ref, hid_ref, wg_ref, wu_ref, wd_ref, rows_ref, sems, out_sems,
    *, n_tp, per_part, width,
):
    rows = x_ref.shape[0]
    sub = arr_ref.shape[1]
    half = sub * LANES
    sources = rows // per_part
    copies = []
    for i, (src, dst) in enumerate(
        ((wg0, wg_ref.at[0]), (wu0, wu_ref.at[0]), (wg1, wg_ref.at[1]), (wu1, wu_ref.at[1]),
         (wd0, wd_ref.at[0]), (wd1, wd_ref.at[1]))
    ):
        copy = pltpu.make_async_copy(src.at[0], dst, sems.at[i])
        copy.start()
        copies.append(copy)

    unit = 20
    pieces = per_part // unit

    def spread(i, carry):
        s, p = i // pieces, i % pieces
        for c in range(n_tp):
            part = arr_ref[pl.ds((s * n_tp + c) * per_part + p * unit, unit)].astype(jnp.float32)
            at = pl.multiple_of(i * (unit * sub), unit * sub)
            tiles_ref[c, pl.ds(at, unit * sub), :] = part.reshape(unit * sub, LANES)
        return carry

    lax.fori_loop(0, sources * pieces, spread, 0)

    block = 80

    def normalize(b, carry):
        def piece(c, j):
            return tiles_ref[c, pl.ds(b * (block * sub) + j, block, stride=sub), :]

        squares = jnp.zeros((block, LANES), jnp.float32)
        for c in range(n_tp):
            for j in range(sub):
                v = piece(c, j)
                squares += v * v
        scale = lax.rsqrt(jnp.sum(squares, axis=1, keepdims=True) / width + EPS)
        at = pl.ds(pl.multiple_of(b * block, block), block)
        for c in range(n_tp):
            for j in range(sub):
                lo = c * half + j * LANES
                v = piece(c, j) * scale * gain_ref[:, lo : lo + LANES]
                x_ref[at, lo : lo + LANES] = v.astype(jnp.bfloat16)
        return carry

    lax.fori_loop(0, rows // block, normalize, 0)

    ff = wg_ref.shape[2]
    step = 256
    for h in range(n_tp):
        copies[2 * h].wait()
        copies[2 * h + 1].wait()
        for n in range(ff // step):
            cols = slice(n * step, (n + 1) * step)
            gate = jnp.dot(x_ref[...], wg_ref[h, :, cols], preferred_element_type=jnp.float32)
            upper = jnp.dot(x_ref[...], wu_ref[h, :, cols], preferred_element_type=jnp.float32)
            hidden = (gate / (1.0 + jnp.exp(-gate))) * upper
            hid_ref[:, h * ff + n * step : h * ff + (n + 1) * step] = hidden.astype(jnp.bfloat16)
    for h in range(n_tp):
        copies[2 * n_tp + h].wait()
    sends = []
    for c in range(n_tp):
        for n in range(half // step):
            lo = c * half + n * step
            total = jnp.dot(
                hid_ref[...],
                jnp.concatenate([wd_ref[h, :, lo : lo + step] for h in range(n_tp)], axis=0),
                preferred_element_type=jnp.float32,
            )
            for i in range(step // LANES):
                j = n * (step // LANES) + i
                tiles_ref[c, pl.ds(j, rows, stride=sub), :] = total[:, i * LANES : (i + 1) * LANES]

        def gather(i, carry):
            s, p = i // pieces, i % pieces
            at = pl.multiple_of(i * (unit * sub), unit * sub)
            part = tiles_ref[c, pl.ds(at, unit * sub), :].reshape(unit, sub, LANES)
            rows_ref[c, s, pl.ds(p * unit, unit)] = part.astype(jnp.bfloat16)
            return carry

        lax.fori_loop(0, sources * pieces, gather, 0)
        sends.append(pltpu.make_async_copy(rows_ref.at[c], out_ref.at[:, c], out_sems.at[c]))
        sends[c].start()
    for send in sends:
        send.wait()


def in_vmem(x):
    return pltpu.with_memory_space_constraint(x, pltpu.VMEM)


def in_hbm(x):
    return pltpu.with_memory_space_constraint(x, pltpu.HBM)


def expert(arrived, gain, gates, uppers, downs, per_part, n_tp):
    total, sub, lanes = arrived.shape
    rows = total // n_tp
    _, width, ff = gates[0].shape
    anywhere = pl.BlockSpec(memory_space=pltpu.HBM)
    return pl.pallas_call(
        functools.partial(expert_kernel, n_tp=n_tp, per_part=per_part, width=width),
        out_shape=pltpu.HBM((rows // per_part, n_tp, per_part, sub, lanes), jnp.bfloat16),
        in_specs=[pl.BlockSpec(memory_space=pltpu.VMEM), pl.BlockSpec(memory_space=pltpu.VMEM)]
        + [anywhere] * (3 * n_tp),
        out_specs=pl.BlockSpec(memory_space=pltpu.HBM),
        scratch_shapes=[
            pltpu.VMEM((n_tp, rows * sub, lanes), jnp.float32),
            pltpu.VMEM((rows, width), jnp.bfloat16),
            pltpu.VMEM((rows, ff * n_tp), jnp.bfloat16),
            pltpu.VMEM((n_tp, width, ff), jnp.bfloat16),
            pltpu.VMEM((n_tp, width, ff), jnp.bfloat16),
            pltpu.VMEM((n_tp, ff, width), jnp.bfloat16),
            pltpu.VMEM((n_tp, rows // per_part, per_part, sub, lanes), jnp.bfloat16),
            pltpu.SemaphoreType.DMA((3 * n_tp,)),
            pltpu.SemaphoreType.DMA((n_tp,)),
        ],
        compiler_params=pltpu.CompilerParams(vmem_limit_bytes=EXPERT_VMEM),
        cost_estimate=pl.CostEstimate(
            flops=6 * rows * width * ff * n_tp, transcendentals=rows * ff * n_tp,
            bytes_accessed=12 * width * ff + 4 * total * sub * lanes,
        ),
        name="expert",
    )(in_vmem(arrived), gain, *[in_hbm(w) for w in (*gates, *uppers, *downs)])


def combine_kernel(pos_ref, mix_ref, *refs):
    *parts, out_ref, sq_ref, ret_ref, tiles_ref, sems = refs
    top, tok_dev = pos_ref.shape
    sub = ret_ref.shape[1]
    block = parts[0].shape[0]
    copies = []
    for i, part in enumerate(parts):
        into = ret_ref.at[pl.ds(i * block, block)]
        copies.append(pltpu.make_async_copy(part, into, sems.at[i]))
    for copy in copies:
        copy.start()
    for copy in copies:
        copy.wait()

    def pick(t, carry):
        total = mix_ref[0, t] * ret_ref[pos_ref[0, t]].astype(jnp.float32)
        for k in range(1, top):
            total += mix_ref[k, t] * ret_ref[pos_ref[k, t]].astype(jnp.float32)
        tiles_ref[pl.ds(pl.multiple_of(t * sub, sub), sub), :] = total
        return carry

    lax.fori_loop(0, tok_dev, pick, 0, unroll=8)
    squares = jnp.zeros((tok_dev, LANES), jnp.float32)
    for j in range(sub):
        v = tiles_ref[pl.ds(j, tok_dev, stride=sub), :]
        out_ref[:, j * LANES : (j + 1) * LANES] = v
        squares += v * v
    sq_ref[...] = jnp.sum(squares, axis=1, keepdims=True)


def combined(pos, mix, returned):
    _, tok_dev = pos.shape
    block, sub, lanes = returned[0].shape
    return pl.pallas_call(
        combine_kernel,
        out_shape=(
            pltpu.VMEM((tok_dev, sub * lanes), jnp.float32),
            jax.ShapeDtypeStruct((tok_dev, 1), jnp.float32),
        ),
        in_specs=[
            pl.BlockSpec(memory_space=pltpu.SMEM),
            pl.BlockSpec(memory_space=pltpu.SMEM),
        ]
        + [pl.BlockSpec(memory_space=pl.ANY)] * len(returned),
        out_specs=(
            pl.BlockSpec(memory_space=pltpu.VMEM),
            pl.BlockSpec(memory_space=pltpu.VMEM),
        ),
        scratch_shapes=[
            pltpu.VMEM((len(returned) * block, sub, lanes), jnp.bfloat16),
            pltpu.VMEM((tok_dev * sub, lanes), jnp.float32),
            pltpu.SemaphoreType.DMA((len(returned),)),
        ],
        compiler_params=pltpu.CompilerParams(vmem_limit_bytes=COMBINE_VMEM),
        name="combine",
    )(pos, mix, *returned)


def finish_kernel(mix_ref, tot_ref, gain_ref, out_ref, *, width):
    totals = jnp.sum(tot_ref[...], axis=0)
    norm = lax.rsqrt(totals / width + EPS)
    out_ref[...] = (mix_ref[...] * norm * gain_ref[...].astype(jnp.float32)).astype(jnp.bfloat16)


def finished(mixed, totals, gain, width):
    return pl.pallas_call(
        functools.partial(finish_kernel, width=width),
        out_shape=jax.ShapeDtypeStruct(mixed.shape, jnp.bfloat16),
        in_specs=[pl.BlockSpec(memory_space=pltpu.VMEM)] * 3,
        out_specs=pl.BlockSpec(memory_space=pltpu.VMEM),
        compiler_params=pltpu.CompilerParams(vmem_limit_bytes=COMBINE_VMEM),
        name="finish",
    )(in_vmem(mixed), totals, gain[None, :])


def body(tokens, norm_gain, w_gate, w_up, w_down, expert_ids, combine, final_gain):
    tok_dev, half = tokens.shape
    n_z = lax.axis_size("z")
    n_tp = lax.axis_size("tp")
    width = half * n_tp
    experts = w_gate.shape[0] * n_z * ROW
    capacity = tok_dev // 8 * 5 * 2 // (experts // GROUPS)
    per_core = capacity // n_tp
    sub = half // LANES
    away = offsets(n_z)
    chunks = (range(NEAR), range(NEAR, n_z))

    def shift(x, by):
        if by % n_z == 0:
            return x
        return lax.ppermute(x, "z", [(i, (i + by) % n_z) for i in range(n_z)])

    def exchange(x):
        return lax.all_to_all(x, ("x", "tp"), split_axis=0, concat_axis=0, tiled=True)

    swap = [(i, (i + 1) % n_tp) for i in range(n_tp)]
    others = []
    for w in (w_gate, w_up, w_down):
        others.append(lax.ppermute(w, "tp", swap))
    gain = lax.all_gather(norm_gain.astype(jnp.float32), "tp", tiled=True)[None, :]
    z = lax.axis_index("z").astype(jnp.int32).reshape(1)
    *outgoing, pos = dispatch(z, expert_ids.T, tokens, experts, capacity)
    came = [shift(x, by) for x, by in zip(outgoing, away)]
    returned = []
    for chunk in chunks:
        parts = [came[i].reshape(ROW * n_tp, per_core, sub, LANES) for i in chunk]
        arrived = exchange(jnp.stack(parts, axis=1))
        results = expert(
            arrived.reshape(-1, sub, LANES), gain, (w_gate, others[0]),
            (w_up, others[1]), (w_down, others[2]), per_core * len(chunk), n_tp,
        )
        back = exchange(results.reshape(arrived.shape))
        for k, i in enumerate(chunk):
            part = back[:, k].reshape(ROW * capacity, sub, LANES)
            returned.append(shift(part, -away[i]))
    mixed, squares = combined(pos, combine.T, returned)
    totals = lax.all_gather(squares, "tp")
    return finished(mixed, totals, final_gain, width)


def solution(mesh):
    grp, ep, tp = mesh.devices.shape
    fine = Mesh(mesh.devices.reshape(grp, ep // ROW, ROW, tp), ("grp", "z", "x", "tp"))
    spot = ("z", "x")
    placed = (
        P(("grp", "z", "x"), "tp"),
        P("tp"),
        P(spot, None, "tp"),
        P(spot, None, "tp"),
        P(spot, "tp", None),
        P(("grp", "z", "x"), None),
        P(("grp", "z", "x"), None),
        P("tp"),
    )
    return jax.shard_map(
        body, mesh=fine, in_specs=placed, out_specs=P(("grp", "z", "x"), "tp"), check_vma=False
    )
```

```python
import functools

import jax
import jax.numpy as jnp
from jax import lax
from jax.experimental import pallas as pl
from jax.experimental.pallas import tpu as pltpu
from jax.sharding import Mesh
from jax.sharding import PartitionSpec as P


GROUPS = 4
ROW = 4
NEAR = 11
EPS = 1e-06
LANES = 128
DISPATCH_VMEM = 60 * 1024 * 1024
EXPERT_VMEM = 40 * 1024 * 1024
COMBINE_VMEM = 8 * 1024 * 1024


def offsets(n_z):
    return [(i + 1) // 2 if i % 2 else -(i // 2) for i in range(n_z)]


def dispatch_kernel(z_ref, ids_ref, tok_ref, *refs, capacity):
    *out_refs, pos_ref, tiles_ref, rows_ref, next_ref, sems = refs
    tok_dev, half = tok_ref.shape
    sub = half // LANES
    top = ids_ref.shape[0]
    n_z = len(out_refs)
    block = ROW * capacity
    for j in range(sub):
        part = tok_ref[:, j * LANES : (j + 1) * LANES].astype(jnp.float32)
        tiles_ref[pl.ds(j, tok_dev, stride=sub), :] = part
    z = z_ref[0]
    for row in range(n_z):
        away = row - z
        away = jnp.where(away < 0, away + n_z, away)
        place_in = jnp.where(away * 2 > n_z, 2 * (n_z - away), jnp.maximum(2 * away - 1, 0))
        for x in range(ROW):
            next_ref[row * ROW + x] = place_in * block + x * capacity

    def place(t, carry):
        row = tiles_ref[pl.ds(pl.multiple_of(t * sub, sub), sub), :].astype(jnp.bfloat16)
        for k in range(top):
            e = ids_ref[k, t]
            slot = next_ref[e]
            next_ref[e] = slot + 1
            pos_ref[k, t] = slot
            rows_ref[slot] = row
        return carry

    lax.fori_loop(0, tok_dev, place, 0, unroll=8)
    copies = []
    for i, out_ref in enumerate(out_refs):
        part = rows_ref.at[pl.ds(i * block, block)]
        copies.append(pltpu.make_async_copy(part, out_ref, sems.at[i]))
    for copy in copies:
        copy.start()
    for copy in copies:
        copy.wait()


def dispatch(z, ids, tokens, experts, capacity):
    tok_dev, half = tokens.shape
    sub = half // LANES
    n_z = experts // ROW
    return pl.pallas_call(
        functools.partial(dispatch_kernel, capacity=capacity),
        out_shape=tuple(
            pltpu.HBM((ROW * capacity, sub, LANES), jnp.bfloat16) for _ in range(n_z)
        )
        + (jax.ShapeDtypeStruct(ids.shape, jnp.int32),),
        in_specs=[
            pl.BlockSpec(memory_space=pltpu.SMEM),
            pl.BlockSpec(memory_space=pltpu.SMEM),
            pl.BlockSpec(memory_space=pltpu.VMEM),
        ],
        out_specs=tuple(pl.BlockSpec(memory_space=pltpu.HBM) for _ in range(n_z))
        + (pl.BlockSpec(memory_space=pltpu.SMEM),),
        scratch_shapes=[
            pltpu.VMEM((tok_dev * sub, LANES), jnp.float32),
            pltpu.VMEM((experts * capacity, sub, LANES), jnp.bfloat16),
            pltpu.SMEM((experts,), jnp.int32),
            pltpu.SemaphoreType.DMA((n_z,)),
        ],
        compiler_params=pltpu.CompilerParams(vmem_limit_bytes=DISPATCH_VMEM),
        name="dispatch",
    )(z, ids, tokens)


def expert_kernel(
    arr_ref, gain_ref, wg0, wg1, wu0, wu1, wd0, wd1, out_ref,
    tiles_ref, x_ref, hid_ref, wg_ref, wu_ref, wd_ref, rows_ref, sems, out_sems,
    *, n_tp, per_part, unit, width,
):
    rows = x_ref.shape[0]
    sub = arr_ref.shape[1]
    half = sub * LANES
    sources = rows // per_part
    copies = []
    for i, (src, dst) in enumerate(
        ((wg0, wg_ref.at[0]), (wu0, wu_ref.at[0]), (wg1, wg_ref.at[1]), (wu1, wu_ref.at[1]),
         (wd0, wd_ref.at[0]), (wd1, wd_ref.at[1]))
    ):
        copy = pltpu.make_async_copy(src.at[0], dst, sems.at[i])
        copy.start()
        copies.append(copy)

    pieces = per_part // unit

    def spread(i, carry):
        s, p = i // pieces, i % pieces
        for c in range(n_tp):
            part = arr_ref[pl.ds((s * n_tp + c) * per_part + p * unit, unit)].astype(jnp.float32)
            at = pl.multiple_of(i * (unit * sub), unit * sub)
            tiles_ref[c, pl.ds(at, unit * sub), :] = part.reshape(unit * sub, LANES)
        return carry

    lax.fori_loop(0, sources * pieces, spread, 0, unroll=2)

    block = 80

    def normalize_at(start, count):
        def piece(c, j):
            return tiles_ref[c, pl.ds(start * sub + j, count, stride=sub), :]

        squares = jnp.zeros((count, LANES), jnp.float32)
        for c in range(n_tp):
            for j in range(sub):
                v = piece(c, j)
                squares += v * v
        scale = lax.rsqrt(jnp.sum(squares, axis=1, keepdims=True) / width + EPS)
        for c in range(n_tp):
            for j in range(sub):
                lo = c * half + j * LANES
                v = piece(c, j) * scale * gain_ref[:, lo : lo + LANES]
                x_ref[pl.ds(start, count), lo : lo + LANES] = v.astype(jnp.bfloat16)

    def normalize(b, carry):
        normalize_at(pl.multiple_of(b * block, block), block)
        return carry

    lax.fori_loop(0, rows // block, normalize, 0)
    if rows % block:
        normalize_at(rows - rows % block, rows % block)

    ff = wg_ref.shape[2]
    step = 256
    per_half = ff // step
    for copy in copies[:2]:
        copy.wait()

    def hidden_block(i, carry):
        h, n = i // per_half, i % per_half

        @pl.when(i == per_half)
        def _():
            for copy in copies[2 : 2 * n_tp]:
                copy.wait()

        cols = pl.ds(pl.multiple_of(n * step, step), step)
        gate = jnp.dot(x_ref[...], wg_ref[h, :, cols], preferred_element_type=jnp.float32)
        upper = jnp.dot(x_ref[...], wu_ref[h, :, cols], preferred_element_type=jnp.float32)
        hidden = (gate / (1.0 + jnp.exp(-gate))) * upper
        hid_ref[:, pl.ds(pl.multiple_of(i * step, step), step)] = hidden.astype(jnp.bfloat16)
        return carry

    lax.fori_loop(0, n_tp * per_half, hidden_block, 0)
    for copy in copies[2 * n_tp :]:
        copy.wait()
    sends = []
    for c in range(n_tp):

        def down_block(n, carry):
            cols = pl.ds(pl.multiple_of(c * half + n * step, step), step)
            total = jnp.dot(
                hid_ref[...],
                jnp.concatenate([wd_ref[h, :, cols] for h in range(n_tp)], axis=0),
                preferred_element_type=jnp.float32,
            )
            for i in range(step // LANES):
                j = n * (step // LANES) + i
                tiles_ref[c, pl.ds(j, rows, stride=sub), :] = total[:, i * LANES : (i + 1) * LANES]
            return carry

        lax.fori_loop(0, half // step, down_block, 0)

        def gather(i, carry):
            s, p = i // pieces, i % pieces
            at = pl.multiple_of(i * (unit * sub), unit * sub)
            part = tiles_ref[c, pl.ds(at, unit * sub), :].reshape(unit, sub, LANES)
            rows_ref[c, s, pl.ds(p * unit, unit)] = part.astype(jnp.bfloat16)
            return carry

        lax.fori_loop(0, sources * pieces, gather, 0, unroll=2)
        sends.append(pltpu.make_async_copy(rows_ref.at[c], out_ref.at[:, c], out_sems.at[c]))
        sends[c].start()
    for send in sends:
        send.wait()


def in_vmem(x):
    return pltpu.with_memory_space_constraint(x, pltpu.VMEM)


def in_hbm(x):
    return pltpu.with_memory_space_constraint(x, pltpu.HBM)


def expert(arrived, gain, gates, uppers, downs, per_part, unit, n_tp):
    total, sub, lanes = arrived.shape
    rows = total // n_tp
    _, width, ff = gates[0].shape
    anywhere = pl.BlockSpec(memory_space=pltpu.HBM)
    return pl.pallas_call(
        functools.partial(
            expert_kernel, n_tp=n_tp, per_part=per_part, unit=unit, width=width
        ),
        out_shape=pltpu.HBM((rows // per_part, n_tp, per_part, sub, lanes), jnp.bfloat16),
        in_specs=[pl.BlockSpec(memory_space=pltpu.VMEM), pl.BlockSpec(memory_space=pltpu.VMEM)]
        + [anywhere] * (3 * n_tp),
        out_specs=pl.BlockSpec(memory_space=pltpu.HBM),
        scratch_shapes=[
            pltpu.VMEM((n_tp, rows * sub, lanes), jnp.float32),
            pltpu.VMEM((rows, width), jnp.bfloat16),
            pltpu.VMEM((rows, ff * n_tp), jnp.bfloat16),
            pltpu.VMEM((n_tp, width, ff), jnp.bfloat16),
            pltpu.VMEM((n_tp, width, ff), jnp.bfloat16),
            pltpu.VMEM((n_tp, ff, width), jnp.bfloat16),
            pltpu.VMEM((n_tp, rows // per_part, per_part, sub, lanes), jnp.bfloat16),
            pltpu.SemaphoreType.DMA((3 * n_tp,)),
            pltpu.SemaphoreType.DMA((n_tp,)),
        ],
        compiler_params=pltpu.CompilerParams(vmem_limit_bytes=EXPERT_VMEM),
        cost_estimate=pl.CostEstimate(
            flops=6 * rows * width * ff * n_tp, transcendentals=rows * ff * n_tp,
            bytes_accessed=12 * width * ff + 4 * total * sub * lanes,
        ),
        name="expert",
    )(in_vmem(arrived), gain, *[in_hbm(w) for w in (*gates, *uppers, *downs)])


def stack_kernel(*refs):
    *parts, out_ref, sems = refs
    copies = [
        pltpu.make_async_copy(part, out_ref.at[:, i], sems.at[i]) for i, part in enumerate(parts)
    ]
    for copy in copies:
        copy.start()
    for copy in copies:
        copy.wait()


def stacked(parts):
    first, *rest = parts[0].shape
    return pl.pallas_call(
        stack_kernel,
        out_shape=pltpu.HBM((first, len(parts), *rest), parts[0].dtype),
        in_specs=[pl.BlockSpec(memory_space=pl.ANY)] * len(parts),
        out_specs=pl.BlockSpec(memory_space=pltpu.HBM),
        scratch_shapes=[pltpu.SemaphoreType.DMA((len(parts),))],
        name="stack",
    )(*parts)


def unstack_kernel(in_ref, *refs):
    *parts, sems = refs
    copies = [
        pltpu.make_async_copy(in_ref.at[:, i], part, sems.at[i]) for i, part in enumerate(parts)
    ]
    for copy in copies:
        copy.start()
    for copy in copies:
        copy.wait()


def unstacked(whole):
    first, count, *rest = whole.shape
    return pl.pallas_call(
        unstack_kernel,
        out_shape=tuple(pltpu.HBM((first, *rest), whole.dtype) for _ in range(count)),
        in_specs=[pl.BlockSpec(memory_space=pl.ANY)],
        out_specs=tuple(pl.BlockSpec(memory_space=pltpu.HBM) for _ in range(count)),
        scratch_shapes=[pltpu.SemaphoreType.DMA((count,))],
        name="unstack",
    )(whole)


def picked(pos_ref, mix_ref, ret_ref, k, t, first):
    at = pos_ref[k, t] - first
    held = (at >= 0) & (at < ret_ref.shape[0])
    row = ret_ref[jnp.where(held, at, 0)].astype(jnp.float32)
    return jnp.where(held, mix_ref[k, t] * row, 0.0)


def fetch(parts, ret_ref, sems):
    block = parts[0].shape[0]
    copies = []
    for i, part in enumerate(parts):
        into = ret_ref.at[pl.ds(i * block, block)]
        copies.append(pltpu.make_async_copy(part, into, sems.at[i]))
    for copy in copies:
        copy.start()
    for copy in copies:
        copy.wait()


def partial_kernel(pos_ref, mix_ref, *refs):
    *parts, out_ref, ret_ref, sems = refs
    top, tok_dev = pos_ref.shape
    sub = ret_ref.shape[1]
    fetch(parts, ret_ref, sems)

    def pick(t, carry):
        total = picked(pos_ref, mix_ref, ret_ref, 0, t, 0)
        for k in range(1, top):
            total += picked(pos_ref, mix_ref, ret_ref, k, t, 0)
        out_ref[pl.ds(pl.multiple_of(t * sub, sub), sub), :] = total
        return carry

    lax.fori_loop(0, tok_dev, pick, 0, unroll=8)


def partial(pos, mix, returned):
    _, tok_dev = pos.shape
    block, sub, lanes = returned[0].shape
    return pl.pallas_call(
        partial_kernel,
        out_shape=pltpu.VMEM((tok_dev * sub, lanes), jnp.float32),
        in_specs=[
            pl.BlockSpec(memory_space=pltpu.SMEM),
            pl.BlockSpec(memory_space=pltpu.SMEM),
        ]
        + [pl.BlockSpec(memory_space=pl.ANY)] * len(returned),
        out_specs=pl.BlockSpec(memory_space=pltpu.VMEM),
        scratch_shapes=[
            pltpu.VMEM((len(returned) * block, sub, lanes), jnp.bfloat16),
            pltpu.SemaphoreType.DMA((len(returned),)),
        ],
        compiler_params=pltpu.CompilerParams(vmem_limit_bytes=COMBINE_VMEM),
        name="partial",
    )(pos, mix, *returned)


def combine_kernel(pos_ref, mix_ref, part_ref, *refs, first):
    *parts, out_ref, sq_ref, ret_ref, tiles_ref, sems = refs
    top, tok_dev = pos_ref.shape
    sub = ret_ref.shape[1]
    fetch(parts, ret_ref, sems)

    def pick(t, carry):
        at = pl.ds(pl.multiple_of(t * sub, sub), sub)
        total = part_ref[at, :]
        for k in range(top):
            total += picked(pos_ref, mix_ref, ret_ref, k, t, first)
        tiles_ref[at, :] = total
        return carry

    lax.fori_loop(0, tok_dev, pick, 0, unroll=8)
    squares = jnp.zeros((tok_dev, LANES), jnp.float32)
    for j in range(sub):
        v = tiles_ref[pl.ds(j, tok_dev, stride=sub), :]
        out_ref[:, j * LANES : (j + 1) * LANES] = v
        squares += v * v
    sq_ref[...] = jnp.sum(squares, axis=1, keepdims=True)


def combined(pos, mix, part, returned, first):
    _, tok_dev = pos.shape
    block, sub, lanes = returned[0].shape
    return pl.pallas_call(
        functools.partial(combine_kernel, first=first),
        out_shape=(
            pltpu.VMEM((tok_dev, sub * lanes), jnp.float32),
            jax.ShapeDtypeStruct((tok_dev, 1), jnp.float32),
        ),
        in_specs=[
            pl.BlockSpec(memory_space=pltpu.SMEM),
            pl.BlockSpec(memory_space=pltpu.SMEM),
            pl.BlockSpec(memory_space=pltpu.VMEM),
        ]
        + [pl.BlockSpec(memory_space=pl.ANY)] * len(returned),
        out_specs=(
            pl.BlockSpec(memory_space=pltpu.VMEM),
            pl.BlockSpec(memory_space=pltpu.VMEM),
        ),
        scratch_shapes=[
            pltpu.VMEM((len(returned) * block, sub, lanes), jnp.bfloat16),
            pltpu.VMEM((tok_dev * sub, lanes), jnp.float32),
            pltpu.SemaphoreType.DMA((len(returned),)),
        ],
        compiler_params=pltpu.CompilerParams(vmem_limit_bytes=COMBINE_VMEM),
        name="combine",
    )(pos, mix, in_vmem(part), *returned)


def finish_kernel(mix_ref, tot_ref, gain_ref, out_ref, *, width):
    totals = jnp.sum(tot_ref[...], axis=0)
    norm = lax.rsqrt(totals / width + EPS)
    out_ref[...] = (mix_ref[...] * norm * gain_ref[...].astype(jnp.float32)).astype(jnp.bfloat16)


def finished(mixed, totals, gain, width):
    return pl.pallas_call(
        functools.partial(finish_kernel, width=width),
        out_shape=jax.ShapeDtypeStruct(mixed.shape, jnp.bfloat16),
        in_specs=[pl.BlockSpec(memory_space=pltpu.VMEM)] * 3,
        out_specs=pl.BlockSpec(memory_space=pltpu.VMEM),
        compiler_params=pltpu.CompilerParams(vmem_limit_bytes=COMBINE_VMEM),
        name="finish",
    )(in_vmem(mixed), totals, gain[None, :])


def body(tokens, norm_gain, w_gate, w_up, w_down, expert_ids, combine, final_gain):
    tok_dev, half = tokens.shape
    n_z = lax.axis_size("z")
    n_tp = lax.axis_size("tp")
    width = half * n_tp
    experts = w_gate.shape[0] * n_z * ROW
    capacity = tok_dev // 8 * 5 * 2 // (experts // GROUPS)
    per_core = capacity // n_tp
    sub = half // LANES
    away = offsets(n_z)
    chunks = (range(NEAR), range(NEAR, n_z))

    def shift(x, by):
        if by % n_z == 0:
            return x
        return lax.ppermute(x, "z", [(i, (i + by) % n_z) for i in range(n_z)])

    def exchange(x):
        return lax.all_to_all(x, ("x", "tp"), split_axis=0, concat_axis=0, tiled=True)

    swap = [(i, (i + 1) % n_tp) for i in range(n_tp)]
    others = []
    for w in (w_gate, w_up, w_down):
        others.append(lax.ppermute(w, "tp", swap))
    gain = lax.all_gather(norm_gain.astype(jnp.float32), "tp", tiled=True)[None, :]
    z = lax.axis_index("z").astype(jnp.int32).reshape(1)
    *outgoing, pos = dispatch(z, expert_ids.T, tokens, experts, capacity)
    came = [shift(x, by) for x, by in zip(outgoing, away)]
    returned = []
    for chunk in chunks:
        parts = [came[i].reshape(ROW * n_tp, per_core, sub, LANES) for i in chunk]
        leaving = stacked(parts)
        arrived = exchange(leaving)
        results = expert(
            arrived.reshape(-1, sub, LANES), gain, (w_gate, others[0]),
            (w_up, others[1]), (w_down, others[2]), per_core * len(chunk), per_core, n_tp,
        )
        back = exchange(results.reshape(arrived.shape))
        parts = unstacked(back)
        parts = [part.reshape(ROW * capacity, sub, LANES) for part in parts]
        returned.append([shift(part, -away[i]) for part, i in zip(parts, chunk)])
    mix = combine.T
    part = partial(pos, mix, returned[0])
    mixed, squares = combined(pos, mix, part, returned[1], NEAR * ROW * capacity)
    totals = lax.all_gather(squares, "tp")
    return finished(mixed, totals, final_gain, width)


def solution(mesh):
    grp, ep, tp = mesh.devices.shape
    fine = Mesh(mesh.devices.reshape(grp, ep // ROW, ROW, tp), ("grp", "z", "x", "tp"))
    spot = ("z", "x")
    placed = (
        P(("grp", "z", "x"), "tp"),
        P("tp"),
        P(spot, None, "tp"),
        P(spot, None, "tp"),
        P(spot, "tp", None),
        P(("grp", "z", "x"), None),
        P(("grp", "z", "x"), None),
        P("tp"),
    )
    return jax.shard_map(
        body, mesh=fine, in_specs=placed, out_specs=P(("grp", "z", "x"), "tp"), check_vma=False
    )
```

```python
import functools

import jax
import jax.numpy as jnp
from jax import lax
from jax.experimental import pallas as pl
from jax.experimental.pallas import tpu as pltpu
from jax.sharding import Mesh
from jax.sharding import PartitionSpec as P


GROUPS = 4
ROW = 4
CUTS = (11,)
EPS = 1e-06
LANES = 128
DISPATCH_VMEM = 60 * 1024 * 1024
EXPERT_VMEM = 40 * 1024 * 1024
COMBINE_VMEM = 8 * 1024 * 1024
SMALL_VMEM = 1024 * 1024


def offsets(n_z):
    return [(i + 1) // 2 if i % 2 else -(i // 2) for i in range(n_z)]


def chunks_of(n_z):
    bounds = (0, *CUTS, n_z)
    return [range(lo, hi) for lo, hi in zip(bounds, bounds[1:])]


def dispatch_kernel(z_ref, ids_ref, tok_ref, *refs, capacity):
    *out_refs, pos_ref, tiles_ref, rows_ref, next_ref, sems = refs
    tok_dev, half = tok_ref.shape
    sub = half // LANES
    top = ids_ref.shape[0]
    n_z = len(out_refs)
    block = ROW * capacity
    for j in range(sub):
        part = tok_ref[:, j * LANES : (j + 1) * LANES].astype(jnp.float32)
        tiles_ref[pl.ds(j, tok_dev, stride=sub), :] = part
    z = z_ref[0]
    for row in range(n_z):
        away = row - z
        away = jnp.where(away < 0, away + n_z, away)
        place_in = jnp.where(away * 2 > n_z, 2 * (n_z - away), jnp.maximum(2 * away - 1, 0))
        for x in range(ROW):
            next_ref[row * ROW + x] = place_in * block + x * capacity

    def place(t, carry):
        row = tiles_ref[pl.ds(pl.multiple_of(t * sub, sub), sub), :].astype(jnp.bfloat16)
        for k in range(top):
            e = ids_ref[k, t]
            slot = next_ref[e]
            next_ref[e] = slot + 1
            pos_ref[k, t] = slot
            rows_ref[slot] = row
        return carry

    lax.fori_loop(0, tok_dev, place, 0, unroll=8)
    copies = []
    for i, out_ref in enumerate(out_refs):
        part = rows_ref.at[pl.ds(i * block, block)]
        copies.append(pltpu.make_async_copy(part, out_ref, sems.at[i]))
    for copy in copies:
        copy.start()
    for copy in copies:
        copy.wait()


def dispatch(z, ids, tokens, experts, capacity):
    tok_dev, half = tokens.shape
    sub = half // LANES
    n_z = experts // ROW
    return pl.pallas_call(
        functools.partial(dispatch_kernel, capacity=capacity),
        out_shape=tuple(
            pltpu.HBM((ROW * capacity, sub, LANES), jnp.bfloat16) for _ in range(n_z)
        )
        + (jax.ShapeDtypeStruct(ids.shape, jnp.int32),),
        in_specs=[
            pl.BlockSpec(memory_space=pltpu.SMEM),
            pl.BlockSpec(memory_space=pltpu.SMEM),
            pl.BlockSpec(memory_space=pltpu.VMEM),
        ],
        out_specs=tuple(pl.BlockSpec(memory_space=pltpu.HBM) for _ in range(n_z))
        + (pl.BlockSpec(memory_space=pltpu.SMEM),),
        scratch_shapes=[
            pltpu.VMEM((tok_dev * sub, LANES), jnp.float32),
            pltpu.VMEM((experts * capacity, sub, LANES), jnp.bfloat16),
            pltpu.SMEM((experts,), jnp.int32),
            pltpu.SemaphoreType.DMA((n_z,)),
        ],
        compiler_params=pltpu.CompilerParams(vmem_limit_bytes=DISPATCH_VMEM),
        name="dispatch",
    )(z, ids, tokens)


def expert_kernel(
    arr_ref, gain_ref, wg0, wg1, wu0, wu1, wd0, wd1, out_ref,
    tiles_ref, x_ref, hid_ref, wg_ref, wu_ref, wd_ref, rows_ref, sems, out_sems,
    *, n_tp, per_part, unit, width,
):
    rows = x_ref.shape[0]
    sub = arr_ref.shape[1]
    half = sub * LANES
    sources = rows // per_part
    copies = []
    for i, (src, dst) in enumerate(
        ((wg0, wg_ref.at[0]), (wu0, wu_ref.at[0]), (wg1, wg_ref.at[1]), (wu1, wu_ref.at[1]),
         (wd0, wd_ref.at[0]), (wd1, wd_ref.at[1]))
    ):
        copy = pltpu.make_async_copy(src.at[0], dst, sems.at[i])
        copy.start()
        copies.append(copy)

    pieces = per_part // unit

    def spread(i, carry):
        s, p = i // pieces, i % pieces
        for c in range(n_tp):
            part = arr_ref[pl.ds((s * n_tp + c) * per_part + p * unit, unit)].astype(jnp.float32)
            at = pl.multiple_of(i * (unit * sub), unit * sub)
            tiles_ref[c, pl.ds(at, unit * sub), :] = part.reshape(unit * sub, LANES)
        return carry

    lax.fori_loop(0, sources * pieces, spread, 0, unroll=2)

    block = 80

    def normalize_at(start, count):
        def piece(c, j):
            return tiles_ref[c, pl.ds(start * sub + j, count, stride=sub), :]

        squares = jnp.zeros((count, LANES), jnp.float32)
        for c in range(n_tp):
            for j in range(sub):
                v = piece(c, j)
                squares += v * v
        scale = lax.rsqrt(jnp.sum(squares, axis=1, keepdims=True) / width + EPS)
        for c in range(n_tp):
            for j in range(sub):
                lo = c * half + j * LANES
                v = piece(c, j) * scale * gain_ref[:, lo : lo + LANES]
                x_ref[pl.ds(start, count), lo : lo + LANES] = v.astype(jnp.bfloat16)

    def normalize(b, carry):
        normalize_at(pl.multiple_of(b * block, block), block)
        return carry

    lax.fori_loop(0, rows // block, normalize, 0)
    if rows % block:
        normalize_at(rows - rows % block, rows % block)

    ff = wg_ref.shape[2]
    step = 256
    per_half = ff // step
    for copy in copies[:2]:
        copy.wait()

    def hidden_block(i, carry):
        h, n = i // per_half, i % per_half

        @pl.when(i == per_half)
        def _():
            for copy in copies[2 : 2 * n_tp]:
                copy.wait()

        cols = pl.ds(pl.multiple_of(n * step, step), step)
        gate = jnp.dot(x_ref[...], wg_ref[h, :, cols], preferred_element_type=jnp.float32)
        upper = jnp.dot(x_ref[...], wu_ref[h, :, cols], preferred_element_type=jnp.float32)
        hidden = (gate / (1.0 + jnp.exp(-gate))) * upper
        hid_ref[:, pl.ds(pl.multiple_of(i * step, step), step)] = hidden.astype(jnp.bfloat16)
        return carry

    lax.fori_loop(0, n_tp * per_half, hidden_block, 0)
    for copy in copies[2 * n_tp :]:
        copy.wait()
    sends = []
    for c in range(n_tp):

        def down_block(n, carry):
            cols = pl.ds(pl.multiple_of(c * half + n * step, step), step)
            total = jnp.dot(
                hid_ref[...],
                jnp.concatenate([wd_ref[h, :, cols] for h in range(n_tp)], axis=0),
                preferred_element_type=jnp.float32,
            )
            for i in range(step // LANES):
                j = n * (step // LANES) + i
                tiles_ref[c, pl.ds(j, rows, stride=sub), :] = total[:, i * LANES : (i + 1) * LANES]
            return carry

        lax.fori_loop(0, half // step, down_block, 0)

        def gather(i, carry):
            s, p = i // pieces, i % pieces
            at = pl.multiple_of(i * (unit * sub), unit * sub)
            part = tiles_ref[c, pl.ds(at, unit * sub), :].reshape(unit, sub, LANES)
            rows_ref[c, s, pl.ds(p * unit, unit)] = part.astype(jnp.bfloat16)
            return carry

        lax.fori_loop(0, sources * pieces, gather, 0, unroll=2)
        sends.append(pltpu.make_async_copy(rows_ref.at[c], out_ref.at[:, c], out_sems.at[c]))
        sends[c].start()
    for send in sends:
        send.wait()


def in_vmem(x):
    return pltpu.with_memory_space_constraint(x, pltpu.VMEM)


def in_hbm(x):
    return pltpu.with_memory_space_constraint(x, pltpu.HBM)


def expert(arrived, gain, gates, uppers, downs, per_part, unit, n_tp):
    total, sub, lanes = arrived.shape
    rows = total // n_tp
    _, width, ff = gates[0].shape
    anywhere = pl.BlockSpec(memory_space=pltpu.HBM)
    return pl.pallas_call(
        functools.partial(
            expert_kernel, n_tp=n_tp, per_part=per_part, unit=unit, width=width
        ),
        out_shape=pltpu.HBM((rows // per_part, n_tp, per_part, sub, lanes), jnp.bfloat16),
        in_specs=[pl.BlockSpec(memory_space=pltpu.VMEM), pl.BlockSpec(memory_space=pltpu.VMEM)]
        + [anywhere] * (3 * n_tp),
        out_specs=pl.BlockSpec(memory_space=pltpu.HBM),
        scratch_shapes=[
            pltpu.VMEM((n_tp, rows * sub, lanes), jnp.float32),
            pltpu.VMEM((rows, width), jnp.bfloat16),
            pltpu.VMEM((rows, ff * n_tp), jnp.bfloat16),
            pltpu.VMEM((n_tp, width, ff), jnp.bfloat16),
            pltpu.VMEM((n_tp, width, ff), jnp.bfloat16),
            pltpu.VMEM((n_tp, ff, width), jnp.bfloat16),
            pltpu.VMEM((n_tp, rows // per_part, per_part, sub, lanes), jnp.bfloat16),
            pltpu.SemaphoreType.DMA((3 * n_tp,)),
            pltpu.SemaphoreType.DMA((n_tp,)),
        ],
        compiler_params=pltpu.CompilerParams(vmem_limit_bytes=EXPERT_VMEM),
        cost_estimate=pl.CostEstimate(
            flops=6 * rows * width * ff * n_tp, transcendentals=rows * ff * n_tp,
            bytes_accessed=12 * width * ff + 4 * total * sub * lanes,
        ),
        name="expert",
    )(in_vmem(arrived), gain, *[in_hbm(w) for w in (*gates, *uppers, *downs)])


def stack_kernel(*refs):
    *parts, out_ref, sems = refs
    copies = [
        pltpu.make_async_copy(part, out_ref.at[:, i], sems.at[i]) for i, part in enumerate(parts)
    ]
    for copy in copies:
        copy.start()
    for copy in copies:
        copy.wait()


def stacked(parts):
    first, *rest = parts[0].shape
    return pl.pallas_call(
        stack_kernel,
        out_shape=pltpu.HBM((first, len(parts), *rest), parts[0].dtype),
        in_specs=[pl.BlockSpec(memory_space=pltpu.VMEM)] * len(parts),
        out_specs=pl.BlockSpec(memory_space=pltpu.HBM),
        scratch_shapes=[pltpu.SemaphoreType.DMA((len(parts),))],
        compiler_params=pltpu.CompilerParams(vmem_limit_bytes=SMALL_VMEM),
        name="stack",
    )(*[in_vmem(part) for part in parts])


def unstack_kernel(in_ref, *refs):
    *parts, sems = refs
    copies = [
        pltpu.make_async_copy(in_ref.at[:, i], part, sems.at[i]) for i, part in enumerate(parts)
    ]
    for copy in copies:
        copy.start()
    for copy in copies:
        copy.wait()


def unstacked(whole):
    first, count, *rest = whole.shape
    return pl.pallas_call(
        unstack_kernel,
        out_shape=tuple(pltpu.HBM((first, *rest), whole.dtype) for _ in range(count)),
        in_specs=[pl.BlockSpec(memory_space=pltpu.VMEM)],
        out_specs=tuple(pl.BlockSpec(memory_space=pltpu.HBM) for _ in range(count)),
        scratch_shapes=[pltpu.SemaphoreType.DMA((count,))],
        compiler_params=pltpu.CompilerParams(vmem_limit_bytes=SMALL_VMEM),
        name="unstack",
    )(in_vmem(whole))


def picked(pos_ref, mix_ref, ret_ref, k, t, first):
    at = pos_ref[k, t] - first
    held = (at >= 0) & (at < ret_ref.shape[0])
    row = ret_ref[jnp.where(held, at, 0)].astype(jnp.float32)
    return jnp.where(held, mix_ref[k, t] * row, 0.0)


def fetch(parts, ret_ref):
    block = parts[0].shape[0]
    for i, part in enumerate(parts):
        ret_ref[i * block : (i + 1) * block] = part[...]


def partial_kernel(pos_ref, mix_ref, *refs):
    *parts, out_ref, ret_ref = refs
    top, tok_dev = pos_ref.shape
    sub = ret_ref.shape[1]
    fetch(parts, ret_ref)

    def pick(t, carry):
        total = picked(pos_ref, mix_ref, ret_ref, 0, t, 0)
        for k in range(1, top):
            total += picked(pos_ref, mix_ref, ret_ref, k, t, 0)
        out_ref[pl.ds(pl.multiple_of(t * sub, sub), sub), :] = total
        return carry

    lax.fori_loop(0, tok_dev, pick, 0, unroll=8)


def partial(pos, mix, returned):
    _, tok_dev = pos.shape
    block, sub, lanes = returned[0].shape
    return pl.pallas_call(
        partial_kernel,
        out_shape=pltpu.VMEM((tok_dev * sub, lanes), jnp.float32),
        in_specs=[
            pl.BlockSpec(memory_space=pltpu.SMEM),
            pl.BlockSpec(memory_space=pltpu.SMEM),
        ]
        + [pl.BlockSpec(memory_space=pltpu.VMEM)] * len(returned),
        out_specs=pl.BlockSpec(memory_space=pltpu.VMEM),
        scratch_shapes=[
            pltpu.VMEM((len(returned) * block, sub, lanes), jnp.bfloat16),
        ],
        compiler_params=pltpu.CompilerParams(vmem_limit_bytes=COMBINE_VMEM),
        name="partial",
    )(pos, mix, *[in_vmem(x) for x in returned])


def combine_kernel(pos_ref, mix_ref, part_ref, *refs, first):
    *parts, out_ref, sq_ref, ret_ref, tiles_ref = refs
    top, tok_dev = pos_ref.shape
    sub = ret_ref.shape[1]
    fetch(parts, ret_ref)

    def pick(t, carry):
        at = pl.ds(pl.multiple_of(t * sub, sub), sub)
        total = part_ref[at, :]
        for k in range(top):
            total += picked(pos_ref, mix_ref, ret_ref, k, t, first)
        tiles_ref[at, :] = total
        return carry

    lax.fori_loop(0, tok_dev, pick, 0, unroll=8)
    squares = jnp.zeros((tok_dev, LANES), jnp.float32)
    for j in range(sub):
        v = tiles_ref[pl.ds(j, tok_dev, stride=sub), :]
        out_ref[:, j * LANES : (j + 1) * LANES] = v
        squares += v * v
    sq_ref[...] = jnp.sum(squares, axis=1, keepdims=True)


def combined(pos, mix, part, returned, first):
    _, tok_dev = pos.shape
    block, sub, lanes = returned[0].shape
    return pl.pallas_call(
        functools.partial(combine_kernel, first=first),
        out_shape=(
            pltpu.VMEM((tok_dev, sub * lanes), jnp.float32),
            jax.ShapeDtypeStruct((tok_dev, 1), jnp.float32),
        ),
        in_specs=[
            pl.BlockSpec(memory_space=pltpu.SMEM),
            pl.BlockSpec(memory_space=pltpu.SMEM),
            pl.BlockSpec(memory_space=pltpu.VMEM),
        ]
        + [pl.BlockSpec(memory_space=pltpu.VMEM)] * len(returned),
        out_specs=(
            pl.BlockSpec(memory_space=pltpu.VMEM),
            pl.BlockSpec(memory_space=pltpu.VMEM),
        ),
        scratch_shapes=[
            pltpu.VMEM((len(returned) * block, sub, lanes), jnp.bfloat16),
            pltpu.VMEM((tok_dev * sub, lanes), jnp.float32),
        ],
        compiler_params=pltpu.CompilerParams(vmem_limit_bytes=COMBINE_VMEM),
        name="combine",
    )(pos, mix, in_vmem(part), *[in_vmem(x) for x in returned])


def finish_kernel(mix_ref, tot_ref, gain_ref, out_ref, *, width):
    totals = jnp.sum(tot_ref[...], axis=0)
    norm = lax.rsqrt(totals / width + EPS)
    out_ref[...] = (mix_ref[...] * norm * gain_ref[...].astype(jnp.float32)).astype(jnp.bfloat16)


def finished(mixed, totals, gain, width):
    return pl.pallas_call(
        functools.partial(finish_kernel, width=width),
        out_shape=jax.ShapeDtypeStruct(mixed.shape, jnp.bfloat16),
        in_specs=[pl.BlockSpec(memory_space=pltpu.VMEM)] * 3,
        out_specs=pl.BlockSpec(memory_space=pltpu.VMEM),
        compiler_params=pltpu.CompilerParams(vmem_limit_bytes=COMBINE_VMEM),
        name="finish",
    )(in_vmem(mixed), totals, gain[None, :])


def body(tokens, norm_gain, w_gate, w_up, w_down, expert_ids, combine, final_gain):
    tok_dev, half = tokens.shape
    n_z = lax.axis_size("z")
    n_tp = lax.axis_size("tp")
    width = half * n_tp
    experts = w_gate.shape[0] * n_z * ROW
    capacity = tok_dev // 8 * 5 * 2 // (experts // GROUPS)
    per_core = capacity // n_tp
    sub = half // LANES
    away = offsets(n_z)
    chunks = chunks_of(n_z)

    def shift(x, by):
        if by % n_z == 0:
            return x
        return lax.ppermute(x, "z", [(i, (i + by) % n_z) for i in range(n_z)])

    def exchange(x):
        return lax.all_to_all(x, ("x", "tp"), split_axis=0, concat_axis=0, tiled=True)

    swap = [(i, (i + 1) % n_tp) for i in range(n_tp)]
    others = []
    for w in (w_gate, w_up, w_down):
        others.append(lax.ppermute(w, "tp", swap))
    gain = lax.all_gather(norm_gain.astype(jnp.float32), "tp", tiled=True)[None, :]
    z = lax.axis_index("z").astype(jnp.int32).reshape(1)
    *outgoing, pos = dispatch(z, expert_ids.T, tokens, experts, capacity)
    came = [shift(x, by) for x, by in zip(outgoing, away)]
    returned = []
    for chunk in chunks:
        parts = [came[i].reshape(ROW * n_tp, per_core, sub, LANES) for i in chunk]
        leaving = stacked(parts)
        arrived = exchange(leaving)
        results = expert(
            arrived.reshape(-1, sub, LANES), gain, (w_gate, others[0]),
            (w_up, others[1]), (w_down, others[2]), per_core * len(chunk), per_core, n_tp,
        )
        back = exchange(results.reshape(arrived.shape))
        parts = unstacked(back)
        parts = [part.reshape(ROW * capacity, sub, LANES) for part in parts]
        returned.append([shift(part, -away[i]) for part, i in zip(parts, chunk)])
    mix = combine.T
    part = partial(pos, mix, [x for chunk in returned[:-1] for x in chunk])
    mixed, squares = combined(pos, mix, part, returned[-1], CUTS[-1] * ROW * capacity)
    totals = lax.all_gather(squares, "tp")
    return finished(mixed, totals, final_gain, width)


def solution(mesh):
    grp, ep, tp = mesh.devices.shape
    fine = Mesh(mesh.devices.reshape(grp, ep // ROW, ROW, tp), ("grp", "z", "x", "tp"))
    spot = ("z", "x")
    placed = (
        P(("grp", "z", "x"), "tp"),
        P("tp"),
        P(spot, None, "tp"),
        P(spot, None, "tp"),
        P(spot, "tp", None),
        P(("grp", "z", "x"), None),
        P(("grp", "z", "x"), None),
        P("tp"),
    )
    return jax.shard_map(
        body, mesh=fine, in_specs=placed, out_specs=P(("grp", "z", "x"), "tp"), check_vma=False
    )
```
